32 devices in a mesh: sp: 16 (over z, y, x), tp: 2 (over core).
Axes of the slice: x: 2, y: 2, z: 4, core: 2. Of those that a mesh axis runs over, the one named last changes fastest.
Arguments:
- residual: bfloat16 [4096, 2048], P(('sp', 'tp')), may hold values from -6 to 6
- pool_input: bfloat16 [4096, 1024], P('sp', 'tp'), may hold values from -6 to 6
- group_maps: bfloat16 [8, 128, 128], replicated, may hold values from -0.5 to 0.5
- pool_scale: float32 [1024], replicated, may hold values from 0.1 to 1.9
- out_proj: bfloat16 [1024, 2048], replicated, may hold values from -0.1875 to 0.1875
- norm_gain: float32 [2048], replicated, may hold values from 0.1 to 1.9
- shared_gate: bfloat16 [2048, 512], replicated, may hold values from -0.125 to 0.125
- shared_up: bfloat16 [2048, 512], replicated, may hold values from -0.125 to 0.125
- shared_down: bfloat16 [512, 2048], replicated, may hold values from -0.25 to 0.25
- expert_gate: bfloat16 [32, 2048, 512], P(('sp', 'tp')), may hold values from -0.125 to 0.125
- expert_up: bfloat16 [32, 2048, 512], P(('sp', 'tp')), may hold values from -0.125 to 0.125
- expert_down: bfloat16 [32, 512, 2048], P(('sp', 'tp')), may hold values from -0.25 to 0.25
- expert_ids: int32 [4096, 4], P(('sp', 'tp')), may hold values from 0 to 31, all different within a row; in each aligned block of 128 rows (0 to 127, 128 to 255, ...) at most 24 rows name the same one
- route_score: float32 [4096, 4], P(('sp', 'tp')), may hold values from 0.05 to 1
Outputs:
- output: bfloat16 [4096, 2048], P(('sp', 'tp'))
The draws below stay inside these ranges and needn't reach their ends.
Inputs may be any that keep to these rules, and one draw needn't show every extreme that they name: `expert_ids`: each row names 4 different experts; among the 128 rows of one device no expert is named more than 24 times, and in some devices' rows one expert is named exactly 24 times.
All inputs are finite; a program needn't handle non-finite values.
Results may differ from the reference program's by a relative error of at most 0.015.
Values may be sent and summed in bfloat16 or wider, within the bound.
A program may use at most 128 MiB of HBM per device.

```python
import math
import jax
import jax.numpy as jnp
import numpy as np
from jax import lax

D = 2048
POOL_GROUPS = 8
GROUP_WIDTH = 128
EXPERT_HIDDEN = 512
SHARED_HIDDEN = 512
TOPK = 4
TOK_DEV = 128
TOKENS = 4096
POOL = 1024
EXPERTS = 32
CAP = 24


def shard_levels(own_key, shape, shards, least, high):
    def one(position, parts):
        draws = jax.random.uniform(jax.random.fold_in(jax.random.fold_in(own_key, 6), position), (parts,), jnp.float32, least / len(shards), high / len(shards))
        return jnp.repeat(jnp.exp(draws), shape[position] // parts).reshape((-1,) + (1,) * (len(shape) - position - 1))

    gain = one(*shards[0])
    for cut in shards[1:]:
        gain = gain * one(*cut)
    return gain


def shared_out(stream_key, own, number, rows, amount, top, reach, lean):
    ranking = jax.random.permutation(stream_key, amount)
    heavy_load, common = portions_of(amount, rows * top, reach, lean, True), portions_of(amount, rows * top, reach, lean, False)
    places = jnp.arange(amount)

    def named(tallies, rotation):
        used = int((tallies > 0).sum())
        fixed = max(1, used // 4)
        moved = fixed + (places - fixed + rotation * (used - fixed)) % max(1, amount - fixed)
        return jnp.zeros((amount,), jnp.int32).at[ranking[jnp.where(places < fixed, places, moved)]].set(jnp.asarray(tallies, jnp.int32))

    tallies = jnp.where(number % 4 == 0, named(heavy_load, number // 4), named(common, number - number // 4 - 1))
    mixed = jax.random.permutation(jax.random.fold_in(own, 3), amount)
    source_of, taker = mixed[0:amount // 2 * 2:2], mixed[1:amount // 2 * 2:2]
    slack = jnp.minimum(tallies[source_of] - 1, reach - tallies[taker]) // 2
    slack = jnp.where((source_of == ranking[0]) | (taker == ranking[0]) | (tallies[taker] == 0), 0, jnp.maximum(slack, 0))
    moved = jax.random.randint(jax.random.fold_in(own, 4), (amount // 2,), 0, 1 << 20) % (slack + 1)
    tallies = tallies.at[source_of].add(-moved).at[taker].add(moved)
    items = jnp.searchsorted(jnp.cumsum(tallies), jnp.arange(rows * top), side="right").astype(jnp.int32)
    table = items.reshape(top, rows).T
    table = table[jax.random.permutation(jax.random.fold_in(own, 1), rows)]
    rotation = jax.random.randint(jax.random.fold_in(own, 2), (rows, 1), 0, top)
    return jnp.take_along_axis(table, (jnp.arange(top)[None, :] + rotation) % top, axis=1)


def portions_of(count, total, bound, slope, full):
    loads = [(1 << 20) // math.isqrt(rank ** slope) + 1 for rank in range(1, count + 1)]
    largest = bound if full else min(bound, max(-(-total // count), total * loads[0] // sum(loads)))
    least = 1 if total - largest >= count - 1 else 0
    given, rest = [largest] + [least] * (count - 1), total - largest - least * (count - 1)
    while rest > 0:
        free = [i for i in range(1, count) if given[i] < largest] or [i for i in range(1, count) if given[i] < bound]
        mass, budget = sum([loads[i] for i in free]), rest
        for i in free:
            more = min(bound - given[i], max(1, budget * loads[i] // mass), rest)
            given[i] = given[i] + more
            rest = rest - more
    return np.array(given)


def bell_draw(stream_key, shape, spread, bound, shards=(), kind=jnp.bfloat16):
    drawn = spread * jax.random.normal(stream_key, shape, jnp.float32)
    if shards:
        drawn = drawn * shard_levels(stream_key, shape, shards, -0.22, 0.18)
    return jnp.clip(drawn, -bound, bound).astype(kind)


def setup_inputs(seed: int = 0) -> dict:
    keys = jax.random.split(jax.random.key(seed), 15)
    residual = bell_draw(keys[0], (TOKENS, D), 1.0, 6.0, ((0, 32),))
    pool_input = bell_draw(keys[1], (TOKENS, POOL), 1.0, 6.0, ((0, 16), (1, 2)))
    group_maps = bell_draw(keys[2], (POOL_GROUPS, GROUP_WIDTH, GROUP_WIDTH), GROUP_WIDTH ** -0.5, 0.5)
    pool_scale = jnp.clip(1.0 + 0.18 * jax.random.normal(keys[3], (POOL,), jnp.float32), 0.1, 1.9)
    out_proj = bell_draw(keys[4], (POOL, D), POOL ** -0.5, 0.1875)
    norm_gain = jnp.clip(1.0 + 0.18 * jax.random.normal(keys[5], (D,), jnp.float32), 0.1, 1.9)
    shared_gate = bell_draw(keys[6], (D, SHARED_HIDDEN), D ** -0.5, 0.125)
    shared_up = bell_draw(keys[7], (D, SHARED_HIDDEN), D ** -0.5, 0.125)
    shared_down = bell_draw(keys[8], (SHARED_HIDDEN, D), SHARED_HIDDEN ** -0.5, 0.25)
    expert_gate = bell_draw(keys[9], (EXPERTS, D, EXPERT_HIDDEN), D ** -0.5, 0.125, ((0, 32),))
    expert_up = bell_draw(keys[10], (EXPERTS, D, EXPERT_HIDDEN), D ** -0.5, 0.125, ((0, 32),))
    expert_down = bell_draw(keys[11], (EXPERTS, EXPERT_HIDDEN, D), EXPERT_HIDDEN ** -0.5, 0.25, ((0, 32),))
    expert_ids_keys = jax.random.split(jax.random.fold_in(keys[12], 1), TOKENS // TOK_DEV)
    expert_ids_turns = jax.random.permutation(jax.random.fold_in(keys[12], 3), TOKENS // TOK_DEV)
    expert_ids = jax.vmap(lambda own, number: shared_out(jax.random.fold_in(keys[12], 2), own, number, TOK_DEV, EXPERTS, TOPK, CAP, 2))(expert_ids_keys, expert_ids_turns).reshape((TOKENS, TOPK))
    route_score = jnp.clip(0.05 + 0.95 * jax.random.uniform(keys[13], (TOKENS, TOPK), jnp.float32) ** shard_levels(keys[13], (TOKENS, TOPK), ((0, 32),), -0.2, 0.2), 0.05, 1.0)
    return dict(residual=residual, pool_input=pool_input, group_maps=group_maps, pool_scale=pool_scale, out_proj=out_proj, norm_gain=norm_gain, shared_gate=shared_gate, shared_up=shared_up, shared_down=shared_down, expert_gate=expert_gate, expert_up=expert_up, expert_down=expert_down, expert_ids=expert_ids, route_score=route_score)


windows = (2, 4, 8, 16)
epsilon = 1e-06
routed_scale = 2.5

def swiglu(row_block, w_gate, w_up, w_down):
    gate_part = jnp.dot(row_block, w_gate, preferred_element_type=jnp.float32)
    up_part = jnp.dot(row_block, w_up, preferred_element_type=jnp.float32)
    hidden = (jax.nn.silu(gate_part) * up_part).astype(jnp.bfloat16)
    return jnp.dot(hidden, w_down, preferred_element_type=jnp.float32)

def reference(residual, pool_input, group_maps, pool_scale, out_proj, norm_gain, shared_gate, shared_up, shared_down, expert_gate, expert_up, expert_down, expert_ids, route_score):
    length = pool_input.shape[0]
    groups = group_maps.shape[0]
    group_width = group_maps.shape[1]
    input_values = pool_input.astype(jnp.float32).reshape(length, groups, group_width)
    places = jnp.arange(length, dtype=jnp.int32)
    pooled = []
    for group_index in range(groups):
        window_span = windows[group_index % 4]
        group_column = input_values[:, group_index]
        padded = jnp.pad(group_column, ((window_span - 1, 0), (0, 0)))
        running_sum = padded[window_span - 1:]
        for offset_shift in range(1, window_span):
            running_sum = running_sum + padded[window_span - 1 - offset_shift:window_span - 1 - offset_shift + length]
        divisor = jnp.minimum(places + 1, window_span).astype(jnp.float32)[:, None]
        pooled.append(running_sum / divisor)
    pooled = jnp.stack(pooled, axis=1)
    contrast = (pooled - input_values).astype(jnp.bfloat16)
    mapped = jnp.einsum('sgc,gcd->sgd', contrast.astype(jnp.float32), group_maps.astype(jnp.float32))
    mixed_rows = (mapped.reshape(length, groups * group_width) * pool_scale).astype(jnp.bfloat16)
    projected = jnp.dot(mixed_rows, out_proj, preferred_element_type=jnp.float32)
    settled = (residual.astype(jnp.float32) + projected).astype(jnp.bfloat16)
    settled_wide = settled.astype(jnp.float32)
    inverse_rms = lax.rsqrt(lax.optimization_barrier(jnp.mean(settled_wide * settled_wide, axis=-1, keepdims=True)) + epsilon)
    normed = (settled_wide * inverse_rms * norm_gain).astype(jnp.bfloat16)
    shared = swiglu(normed, shared_gate, shared_up, shared_down)
    weights = route_score / lax.optimization_barrier(jnp.sum(route_score, axis=-1, keepdims=True)) * routed_scale
    experts = expert_gate.shape[0]
    top_count = expert_ids.shape[1]
    assigned = length * top_count
    flat_ids = expert_ids.reshape(assigned).astype(jnp.int32)
    sort_order = jnp.argsort(flat_ids, stable=True).astype(jnp.int32)
    sorted_ids = flat_ids[sort_order]
    counts = jnp.bincount(flat_ids, length=experts).astype(jnp.int32)
    starts = jnp.cumsum(counts).astype(jnp.int32) - counts
    expert_depth = EXPERTS * CAP
    slot_rank = jnp.arange(assigned, dtype=jnp.int32) - starts[sorted_ids]
    slot_index = sorted_ids * expert_depth + slot_rank
    slot_token = jnp.zeros((experts * expert_depth,), jnp.int32).at[slot_index].set(sort_order // top_count)
    slot_weight = jnp.zeros((experts * expert_depth,), jnp.float32).at[slot_index].set(weights.reshape(assigned)[sort_order])

    def one_expert(routed, inputs):
        token_index, slot_factor, w_gate, w_up, w_down = inputs
        expert_rows = swiglu(normed[token_index], w_gate, w_up, w_down).astype(jnp.bfloat16)
        return (routed.at[token_index].add(slot_factor[:, None] * expert_rows.astype(jnp.float32)), None)
    routed, _ = lax.scan(one_expert, jnp.zeros((length, D), jnp.float32), (slot_token.reshape(experts, expert_depth), slot_weight.reshape(experts, expert_depth), expert_gate, expert_up, expert_down))
    return (settled_wide + shared + routed).astype(jnp.bfloat16)
```

```python
import functools
import math

import jax
import jax.numpy as jnp
from jax import lax
from jax.experimental import pallas as pl
from jax.experimental.pallas import tpu as pltpu
from jax.sharding import PartitionSpec as P

windows = (2, 4, 8, 16)
epsilon = 1e-06
routed_scale = 2.5


def from_behind(shard, axis, by):
    peers = lax.axis_size(axis)
    pairs = [(i, i + by) for i in range(peers) if 0 <= i + by < peers]
    return lax.ppermute(shard, axis, pairs)


def layer_count(size_sp):
    return max(d for d in range(1, math.isqrt(size_sp) + 1) if size_sp % d == 0)


def moe_kernel(
    layers,
    peers,
    cores,
    cap,
    top,
    normed_ref,
    settled_ref,
    meta_ref,
    sg_hbm,
    su_hbm,
    sd_hbm,
    eg_hbm,
    eu_hbm,
    ed_hbm,
    out_ref,
    gathered,
    metas,
    packed,
    arrived,
    results,
    back,
    part,
    landed,
    acc,
    sg,
    su,
    sd,
    eg,
    eu,
    ed,
    w_sem,
    own_sem,
    z_send,
    z_recv,
    m_send,
    m_recv,
    a_send,
    a_recv,
    b_send,
    b_recv,
    c_send,
    c_recv,
):
    per_layer = peers // cores
    sp = lax.axis_index("sp")
    core = lax.axis_index("tp")
    z = sp // per_layer
    q = sp % per_layer
    me = q * cores + core
    tokens, width = normed_ref.shape
    slots = peers * cap
    step_cols = min(width, 512)

    def in_column(s):
        return (s * per_layer + q, core)

    def in_layer(p):
        return (z * per_layer + p // cores, p % cores)

    def remote(src, dst, send, recv, to):
        return pltpu.make_async_remote_copy(
            src_ref=src,
            dst_ref=dst,
            send_sem=send,
            recv_sem=recv,
            device_id=to,
            device_id_type=pl.DeviceIdType.MESH,
        )

    loads = [
        pltpu.make_async_copy(a, b, w_sem.at[i])
        for i, (a, b) in enumerate(
            (
                (sg_hbm, sg),
                (su_hbm, su),
                (sd_hbm, sd),
                (eg_hbm.at[0], eg),
                (eu_hbm.at[0], eu),
                (ed_hbm.at[0], ed),
            )
        )
    ]
    own_rows = pltpu.make_async_copy(normed_ref, gathered.at[z], own_sem.at[0])
    own_meta = pltpu.make_async_copy(meta_ref, metas.at[z], own_sem.at[1])
    own_rows.start()
    own_meta.start()

    barrier = pltpu.get_barrier_semaphore()
    for o in range(1, layers):
        pl.semaphore_signal(
            barrier, inc=1, device_id=in_column((z + o) % layers),
            device_id_type=pl.DeviceIdType.MESH,
        )
    for o in range(1, peers):
        pl.semaphore_signal(
            barrier, inc=1, device_id=in_layer((me + o) % peers),
            device_id_type=pl.DeviceIdType.MESH,
        )
    pl.semaphore_wait(barrier, layers - 1 + peers - 1)
    own_rows.wait()
    own_meta.wait()

    def meta_copy(target, source):
        return remote(
            metas.at[source], metas.at[source], m_send.at[target], m_recv.at[source],
            in_column(target),
        )

    for o in range(1, layers):
        meta_copy((z + o) % layers, z).start()

    def chunk_copy(s, side):
        to = z + 1 if side == 0 else z - 1
        to = jnp.clip(to, 0, layers - 1)
        return remote(
            gathered.at[s], gathered.at[s], z_send.at[side, s], z_recv.at[s], in_column(to)
        )

    def goes_up(s):
        return jnp.logical_and(s <= z, z < layers - 1)

    def goes_down(s):
        return jnp.logical_and(s >= z, z > 0)

    def pack_copy(s, p, source):
        return remote(
            packed.at[s, p], arrived.at[s, source], a_send.at[s, p], a_recv.at[s, source],
            in_layer(p),
        )

    def back_copy(s, p, source):
        return remote(
            results.at[s, p], back.at[s, source], b_send.at[s, p], b_recv.at[s, source],
            in_layer(p),
        )

    def part_copy(s, source):
        return remote(
            part.at[s], landed.at[source], c_send.at[s], c_recv.at[source], in_column(s)
        )

    def own_pack(s):
        return pltpu.make_async_copy(packed.at[s, me], arrived.at[s, me], a_recv.at[s, me])

    def own_back(s):
        return pltpu.make_async_copy(results.at[s, me], back.at[s, me], b_recv.at[s, me])

    near = jnp.minimum(z, layers - 1 - z)

    def chunk_at(i):
        both = (i + 1) // 2
        two_sided = jnp.where(i % 2 == 1, z - both, z + both)
        one_sided = jnp.where(2 * z <= layers - 1, z + (i - near), z - (i - near))
        return jnp.where(i <= 2 * near, two_sided, one_sided)

    def slot_table(s, value):
        ids = lax.broadcasted_iota(jnp.int32, (slots, tokens), 0).astype(jnp.float32)
        ids = ids + (z * slots).astype(jnp.float32)
        table = jnp.zeros((slots, tokens), jnp.float32)
        rows = metas[s]
        for k in range(top):
            hit = ids == rows[k : k + 1]
            table = table + jnp.where(hit, rows[top + k : top + k + 1] if value else 1.0, 0.0)
        return table

    def dispatch(i):
        s = chunk_at(i)

        @pl.when(i > 0)
        def _():
            chunk_copy(s, 0).wait_recv()

        @pl.when(goes_up(s))
        def _():
            chunk_copy(s, 0).start()

        @pl.when(goes_down(s))
        def _():
            chunk_copy(s, 1).start()

        @pl.when(i > 0)
        def _():
            meta_copy(z, s).wait_recv()

        table = slot_table(s, False).astype(jnp.bfloat16)
        for col in range(0, width, step_cols):
            got = jnp.dot(
                table, gathered[s, :, col : col + step_cols], preferred_element_type=jnp.float32
            )
            packed[s, :, :, col : col + step_cols] = (
                got.astype(jnp.bfloat16).reshape(peers, cap, step_cols)
            )
        for o in range(1, peers):
            pack_copy(s, (me + o) % peers, me).start()
        own_pack(s).start()

    def mlp(rows, w_gate, w_up):
        gate = jnp.dot(rows, w_gate[...], preferred_element_type=jnp.float32)
        up = jnp.dot(rows, w_up[...], preferred_element_type=jnp.float32)
        return (gate / (1.0 + jnp.exp(-gate)) * up).astype(jnp.bfloat16)

    def expert(i):
        s = chunk_at(i)
        for o in range(1, peers):
            p = (me + o) % peers
            pack_copy(s, p, p).wait_recv()
        own_pack(s).wait()
        hidden = mlp(arrived[s].reshape(slots, width), eg, eu)
        for col in range(0, width, step_cols):
            got = jnp.dot(hidden, ed[:, col : col + step_cols], preferred_element_type=jnp.float32)
            results[s, :, :, col : col + step_cols] = (
                got.astype(jnp.bfloat16).reshape(peers, cap, step_cols)
            )
        for o in range(1, peers):
            back_copy(s, (me + o) % peers, me).start()
        own_back(s).start()

    def combine(i):
        s = chunk_at(i)
        for o in range(1, peers):
            p = (me + o) % peers
            back_copy(s, p, p).wait_recv()
        own_back(s).wait()
        table = slot_table(s, True)
        high = table.astype(jnp.bfloat16)
        low = (table - high.astype(jnp.float32)).astype(jnp.bfloat16)
        dims = (((0,), (0,)), ((), ()))
        for col in range(0, width, step_cols):
            rows = back[s, :, :, col : col + step_cols].reshape(slots, step_cols)
            got = lax.dot_general(high, rows, dims, preferred_element_type=jnp.float32)
            got = got + lax.dot_general(low, rows, dims, preferred_element_type=jnp.float32)

            @pl.when(i == 0)
            def _():
                acc[:, col : col + step_cols] = acc[:, col : col + step_cols] + got

            @pl.when(i > 0)
            def _():
                part[s, :, col : col + step_cols] = got.astype(jnp.bfloat16)

        @pl.when(i > 0)
        def _():
            part_copy(s, z).start()

    def shared():
        for load in loads:
            load.wait()
        hidden = mlp(normed_ref[...], sg, su)
        for col in range(0, width, step_cols):
            got = jnp.dot(hidden, sd[:, col : col + step_cols], preferred_element_type=jnp.float32)
            acc[:, col : col + step_cols] = got + settled_ref[:, col : col + step_cols].astype(
                jnp.float32
            )

    def step(i, carry):
        @pl.when(i < layers)
        def _():
            dispatch(i)

        @pl.when(i == 0)
        def _():
            shared()

        @pl.when(jnp.logical_and(i >= 1, i <= layers))
        def _():
            expert(i - 1)

        @pl.when(i >= 2)
        def _():
            combine(i - 2)

        return carry

    for load in loads:
        load.start()
    lax.fori_loop(0, layers + 2, step, 0)

    def drain(s, carry):
        @pl.when(goes_up(s))
        def _():
            chunk_copy(s, 0).wait_send()

        @pl.when(goes_down(s))
        def _():
            chunk_copy(s, 1).wait_send()

        for o in range(1, peers):
            p = (me + o) % peers
            pack_copy(s, p, me).wait_send()
            back_copy(s, p, me).wait_send()
        return carry

    lax.fori_loop(0, layers, drain, 0)
    for o in range(1, layers):
        s = (z + o) % layers
        meta_copy(s, z).wait_send()
        part_copy(s, z).wait_send()
        part_copy(s, s).wait_recv()
    for col in range(0, width, step_cols):
        total = acc[:, col : col + step_cols]
        for o in range(1, layers):
            s = (z + o) % layers
            total = total + landed[s, :, col : col + step_cols].astype(jnp.float32)
        out_ref[:, col : col + step_cols] = total.astype(jnp.bfloat16)


def on_device(
    residual,
    pool_input,
    group_maps,
    pool_scale,
    out_proj,
    norm_gain,
    shared_gate,
    shared_up,
    shared_down,
    expert_gate,
    expert_up,
    expert_down,
    expert_ids,
    route_score,
):
    row_count, channels = pool_input.shape
    group_width = group_maps.shape[1]
    groups_here = channels // group_width
    halo_reach = max(windows) - 1
    before = from_behind(pool_input[row_count - halo_reach :], "sp", 1)
    extended = (
        jnp.concatenate([before, pool_input], axis=0)
        .astype(jnp.float32)
        .reshape(row_count + halo_reach, groups_here, group_width)
    )
    places = lax.axis_index("sp") * row_count + jnp.arange(row_count, dtype=jnp.int32)
    pooled = []
    for group_index in range(groups_here):
        running_sum = extended[:, group_index]
        window_span = 1
        while window_span < windows[group_index % 4]:
            running_sum = running_sum[window_span:] + running_sum[:-window_span]
            window_span = window_span * 2
        divisor = jnp.minimum(places + 1, window_span).astype(jnp.float32)[:, None]
        pooled.append(running_sum[running_sum.shape[0] - row_count :] / divisor)
    pooled = jnp.stack(pooled, axis=1)
    contrast = (pooled - extended[halo_reach:]).astype(jnp.bfloat16)
    first_group = lax.axis_index("tp") * groups_here
    maps_here = lax.dynamic_slice_in_dim(group_maps, first_group, groups_here, 0)
    mapped = jnp.einsum("sgc,gcd->sgd", contrast, maps_here, preferred_element_type=jnp.float32)
    scale_here = lax.dynamic_slice_in_dim(pool_scale, first_group * group_width, channels, 0)
    mixed_rows = (mapped.reshape(row_count, channels) * scale_here).astype(jnp.bfloat16)
    model_width = out_proj.shape[1]
    swapped = lax.all_to_all(mixed_rows, "tp", split_axis=0, concat_axis=1, tiled=True)
    projected = jnp.dot(swapped, out_proj, preferred_element_type=jnp.float32)
    settled = (residual.astype(jnp.float32) + projected).astype(jnp.bfloat16)
    settled_wide = settled.astype(jnp.float32)
    inverse_rms = lax.rsqrt(jnp.mean(settled_wide * settled_wide, axis=-1, keepdims=True) + epsilon)
    normed = (settled_wide * inverse_rms * norm_gain).astype(jnp.bfloat16)
    tokens_here, top_count = expert_ids.shape
    size_sp = lax.axis_size("sp")
    size_tp = lax.axis_size("tp")
    experts = size_sp * size_tp
    capacity = 3 * tokens_here * top_count // (2 * experts)
    cap = -(-capacity // 8) * 8
    layers = layer_count(size_sp)
    peers = experts // layers
    assigned = tokens_here * top_count
    flat_ids = expert_ids.reshape(assigned)
    onehot = (flat_ids[:, None] == jnp.arange(experts, dtype=jnp.int32)[None, :]).astype(
        jnp.bfloat16
    )
    earlier = (jnp.arange(assigned)[None, :] < jnp.arange(assigned)[:, None]).astype(jnp.bfloat16)
    before_counts = jnp.dot(earlier, onehot, preferred_element_type=jnp.float32)
    position = jnp.sum(before_counts * onehot, axis=1)
    slot = (flat_ids.astype(jnp.float32) * cap + position).reshape(tokens_here, top_count)
    weights = route_score / jnp.sum(route_score, axis=-1, keepdims=True) * routed_scale
    meta = jnp.concatenate([slot, weights], axis=1).T
    hidden_width = shared_gate.shape[1]
    expert_width = expert_gate.shape[2]
    any_spec = pl.BlockSpec(memory_space=pl.ANY)
    vmem_spec = pl.BlockSpec(memory_space=pltpu.VMEM)
    bf16, f32 = jnp.bfloat16, jnp.float32
    dma = pltpu.SemaphoreType.DMA
    routed = (layers, peers, cap, model_width)
    chunks = (layers, tokens_here, model_width)
    return pl.pallas_call(
        functools.partial(moe_kernel, layers, peers, size_tp, cap, top_count),
        out_shape=jax.ShapeDtypeStruct((tokens_here, model_width), bf16),
        in_specs=[vmem_spec] * 3 + [any_spec] * 6,
        out_specs=vmem_spec,
        scratch_shapes=[
            pltpu.VMEM(chunks, bf16),
            pltpu.VMEM((layers, 2 * top_count, tokens_here), f32),
            pltpu.VMEM(routed, bf16),
            pltpu.VMEM(routed, bf16),
            pltpu.VMEM(routed, bf16),
            pltpu.VMEM(routed, bf16),
            pltpu.VMEM(chunks, bf16),
            pltpu.VMEM(chunks, bf16),
            pltpu.VMEM((tokens_here, model_width), f32),
            pltpu.VMEM((model_width, hidden_width), bf16),
            pltpu.VMEM((model_width, hidden_width), bf16),
            pltpu.VMEM((hidden_width, model_width), bf16),
            pltpu.VMEM((model_width, expert_width), bf16),
            pltpu.VMEM((model_width, expert_width), bf16),
            pltpu.VMEM((expert_width, model_width), bf16),
            dma((6,)),
            dma((2,)),
            dma((2, layers)),
            dma((layers,)),
            dma((layers,)),
            dma((layers,)),
            dma((layers, peers)),
            dma((layers, peers)),
            dma((layers, peers)),
            dma((layers, peers)),
            dma((layers,)),
            dma((layers,)),
        ],
        compiler_params=pltpu.CompilerParams(
            collective_id=0, has_side_effects=True, vmem_limit_bytes=58 * 1024 * 1024
        ),
    )(
        normed,
        settled,
        meta,
        shared_gate,
        shared_up,
        shared_down,
        expert_gate,
        expert_up,
        expert_down,
    )


def solution(mesh):
    in_specs = (
        P(("sp", "tp"), None),
        P("sp", "tp"),
        P(),
        P(),
        P(),
        P(),
        P(),
        P(),
        P(),
        P(("sp", "tp"), None, None),
        P(("sp", "tp"), None, None),
        P(("sp", "tp"), None, None),
        P(("sp", "tp"), None),
        P(("sp", "tp"), None),
    )
    out_specs = P(("sp", "tp"), None)
    return jax.shard_map(
        on_device, mesh=mesh, in_specs=in_specs, out_specs=out_specs, check_vma=False
    )
```

```python
import functools
import math

import jax
import jax.numpy as jnp
from jax import lax
from jax.experimental import pallas as pl
from jax.experimental.pallas import tpu as pltpu
from jax.sharding import PartitionSpec as P

windows = (2, 4, 8, 16)
epsilon = 1e-06
routed_scale = 2.5


def from_behind(shard, axis, by):
    peers = lax.axis_size(axis)
    pairs = [(i, i + by) for i in range(peers) if 0 <= i + by < peers]
    return lax.ppermute(shard, axis, pairs)


def layer_count(size_sp):
    return max(d for d in range(1, math.isqrt(size_sp) + 1) if size_sp % d == 0)


def moe_kernel(
    layers,
    peers,
    cores,
    cap,
    top,
    normed_ref,
    settled_ref,
    meta_ref,
    sg_hbm,
    su_hbm,
    sd_hbm,
    eg_hbm,
    eu_hbm,
    ed_hbm,
    out_ref,
    gathered,
    metas,
    packed,
    arrived,
    results,
    back,
    part,
    landed,
    acc,
    sg,
    su,
    sd,
    eg,
    eu,
    ed,
    w_sem,
    own_sem,
    z_send,
    z_recv,
    m_send,
    m_recv,
    a_send,
    a_recv,
    b_send,
    b_recv,
    c_send,
    c_recv,
):
    per_layer = peers // cores
    sp = lax.axis_index("sp")
    core = lax.axis_index("tp")
    z = sp // per_layer
    q = sp % per_layer
    me = q * cores + core
    tokens, width = normed_ref.shape
    slots = peers * cap
    step_cols = min(width, 512)

    def in_column(s):
        return (s * per_layer + q, core)

    def in_layer(p):
        return (z * per_layer + p // cores, p % cores)

    def remote(src, dst, send, recv, to):
        return pltpu.make_async_remote_copy(
            src_ref=src,
            dst_ref=dst,
            send_sem=send,
            recv_sem=recv,
            device_id=to,
            device_id_type=pl.DeviceIdType.MESH,
        )

    loads = [
        pltpu.make_async_copy(a, b, w_sem.at[i])
        for i, (a, b) in enumerate(
            (
                (sg_hbm, sg),
                (su_hbm, su),
                (sd_hbm, sd),
                (eg_hbm.at[0], eg),
                (eu_hbm.at[0], eu),
                (ed_hbm.at[0], ed),
            )
        )
    ]
    own_rows = pltpu.make_async_copy(normed_ref, gathered.at[z], own_sem.at[0])
    own_meta = pltpu.make_async_copy(meta_ref, metas.at[z], own_sem.at[1])
    own_rows.start()
    own_meta.start()
    for load in loads:
        load.start()

    barrier = pltpu.get_barrier_semaphore()
    for o in range(1, layers):
        pl.semaphore_signal(
            barrier, inc=1, device_id=in_column((z + o) % layers),
            device_id_type=pl.DeviceIdType.MESH,
        )
    for o in range(1, peers):
        pl.semaphore_signal(
            barrier, inc=1, device_id=in_layer((me + o) % peers),
            device_id_type=pl.DeviceIdType.MESH,
        )
    pl.semaphore_wait(barrier, layers - 1 + peers - 1)
    own_rows.wait()
    own_meta.wait()

    def meta_copy(target, source):
        return remote(
            metas.at[source], metas.at[source], m_send.at[target], m_recv.at[source],
            in_column(target),
        )

    for o in range(1, layers):
        meta_copy((z + o) % layers, z).start()

    def chunk_copy(s, side):
        to = z + 1 if side == 0 else z - 1
        to = jnp.clip(to, 0, layers - 1)
        return remote(
            gathered.at[s], gathered.at[s], z_send.at[side, s], z_recv.at[s], in_column(to)
        )

    def goes_up(s):
        return jnp.logical_and(s <= z, z < layers - 1)

    def goes_down(s):
        return jnp.logical_and(s >= z, z > 0)

    def pack_copy(s, p, source):
        return remote(
            packed.at[s, p], arrived.at[s, source], a_send.at[s, p], a_recv.at[s, source],
            in_layer(p),
        )

    def back_copy(s, p, source):
        return remote(
            results.at[s, p], back.at[s, source], b_send.at[s, p], b_recv.at[s, source],
            in_layer(p),
        )

    def part_copy(s, source):
        return remote(
            part.at[s], landed.at[source], c_send.at[s], c_recv.at[source], in_column(s)
        )

    def own_pack(s):
        return pltpu.make_async_copy(packed.at[s, me], arrived.at[s, me], a_recv.at[s, me])

    def own_back(s):
        return pltpu.make_async_copy(results.at[s, me], back.at[s, me], b_recv.at[s, me])

    near = jnp.minimum(z, layers - 1 - z)

    def chunk_at(i):
        both = (i + 1) // 2
        two_sided = jnp.where(i % 2 == 1, z - both, z + both)
        one_sided = jnp.where(2 * z <= layers - 1, z + (i - near), z - (i - near))
        return jnp.where(i <= 2 * near, two_sided, one_sided)

    def slot_table(s, value):
        ids = lax.broadcasted_iota(jnp.int32, (slots, tokens), 0).astype(jnp.float32)
        ids = ids + (z * slots).astype(jnp.float32)
        table = jnp.zeros((slots, tokens), jnp.float32)
        rows = metas[s]
        for k in range(top):
            hit = ids == rows[k : k + 1]
            table = table + jnp.where(hit, rows[top + k : top + k + 1] if value else 1.0, 0.0)
        return table

    def dispatch(i):
        s = chunk_at(i)

        @pl.when(i > 0)
        def _():
            chunk_copy(s, 0).wait_recv()

        @pl.when(goes_up(s))
        def _():
            chunk_copy(s, 0).start()

        @pl.when(goes_down(s))
        def _():
            chunk_copy(s, 1).start()

        @pl.when(i > 0)
        def _():
            meta_copy(z, s).wait_recv()

        table = slot_table(s, False).astype(jnp.bfloat16)
        for col in range(0, width, step_cols):
            got = jnp.dot(
                table, gathered[s, :, col : col + step_cols], preferred_element_type=jnp.float32
            )
            packed[s, :, :, col : col + step_cols] = (
                got.astype(jnp.bfloat16).reshape(peers, cap, step_cols)
            )
        for o in range(1, peers):
            pack_copy(s, (me + o) % peers, me).start()
        own_pack(s).start()

    def mlp(rows, w_gate, w_up):
        gate = jnp.dot(rows, w_gate[...], preferred_element_type=jnp.float32)
        up = jnp.dot(rows, w_up[...], preferred_element_type=jnp.float32)
        return (gate / (1.0 + jnp.exp(-gate)) * up).astype(jnp.bfloat16)

    def expert(i):
        s = chunk_at(i)
        for o in range(1, peers):
            p = (me + o) % peers
            pack_copy(s, p, p).wait_recv()
        own_pack(s).wait()
        hidden = mlp(arrived[s].reshape(slots, width), eg, eu)
        for col in range(0, width, step_cols):
            got = jnp.dot(hidden, ed[:, col : col + step_cols], preferred_element_type=jnp.float32)
            results[s, :, :, col : col + step_cols] = (
                got.astype(jnp.bfloat16).reshape(peers, cap, step_cols)
            )
        for o in range(1, peers):
            back_copy(s, (me + o) % peers, me).start()
        own_back(s).start()

    def combine(i):
        s = chunk_at(i)
        for o in range(1, peers):
            p = (me + o) % peers
            back_copy(s, p, p).wait_recv()
        own_back(s).wait()
        table = slot_table(s, True)
        high = table.astype(jnp.bfloat16)
        low = (table - high.astype(jnp.float32)).astype(jnp.bfloat16)
        dims = (((0,), (0,)), ((), ()))
        for col in range(0, width, step_cols):
            rows = back[s, :, :, col : col + step_cols].reshape(slots, step_cols)
            got = lax.dot_general(high, rows, dims, preferred_element_type=jnp.float32)
            got = got + lax.dot_general(low, rows, dims, preferred_element_type=jnp.float32)

            @pl.when(i == 0)
            def _():
                acc[:, col : col + step_cols] = acc[:, col : col + step_cols] + got

            @pl.when(i > 0)
            def _():
                part[s, :, col : col + step_cols] = got.astype(jnp.bfloat16)

        @pl.when(i > 0)
        def _():
            part_copy(s, z).start()

    def shared():
        for load in loads[:3]:
            load.wait()
        hidden = mlp(normed_ref[...], sg, su)
        for col in range(0, width, step_cols):
            got = jnp.dot(hidden, sd[:, col : col + step_cols], preferred_element_type=jnp.float32)
            acc[:, col : col + step_cols] = got + settled_ref[:, col : col + step_cols].astype(
                jnp.float32
            )

    at_end = near == 0

    def step(i, carry):
        later = jnp.logical_and(i >= 3, at_end)

        @pl.when(later)
        def _():
            combine(i - 2)

        @pl.when(i < layers)
        def _():
            dispatch(i)

        @pl.when(i >= 2)
        def _():
            expert(i - 1)

        @pl.when(jnp.logical_and(i >= 3, jnp.logical_not(at_end)))
        def _():
            combine(i - 2)

        return carry

    def last(j, carry):
        combine((layers - 1) * (1 - j))
        return carry

    dispatch(jnp.int32(0))
    shared()
    for load in loads[3:]:
        load.wait()
    lax.fori_loop(1, layers + 1, step, 0)
    expert(jnp.int32(0))
    lax.fori_loop(0, 2, last, 0)

    def drain(s, carry):
        @pl.when(goes_up(s))
        def _():
            chunk_copy(s, 0).wait_send()

        @pl.when(goes_down(s))
        def _():
            chunk_copy(s, 1).wait_send()

        for o in range(1, peers):
            p = (me + o) % peers
            pack_copy(s, p, me).wait_send()
            back_copy(s, p, me).wait_send()
        return carry

    lax.fori_loop(0, layers, drain, 0)
    for o in range(1, layers):
        s = (z + o) % layers
        meta_copy(s, z).wait_send()
        part_copy(s, z).wait_send()
        part_copy(s, s).wait_recv()
    for col in range(0, width, step_cols):
        total = acc[:, col : col + step_cols]
        for o in range(1, layers):
            s = (z + o) % layers
            total = total + landed[s, :, col : col + step_cols].astype(jnp.float32)
        out_ref[:, col : col + step_cols] = total.astype(jnp.bfloat16)


def on_device(
    residual,
    pool_input,
    group_maps,
    pool_scale,
    out_proj,
    norm_gain,
    shared_gate,
    shared_up,
    shared_down,
    expert_gate,
    expert_up,
    expert_down,
    expert_ids,
    route_score,
):
    row_count, channels = pool_input.shape
    group_width = group_maps.shape[1]
    groups_here = channels // group_width
    halo_reach = max(windows) - 1
    before = from_behind(pool_input[row_count - halo_reach :], "sp", 1)
    extended = (
        jnp.concatenate([before, pool_input], axis=0)
        .astype(jnp.float32)
        .reshape(row_count + halo_reach, groups_here, group_width)
    )
    places = lax.axis_index("sp") * row_count + jnp.arange(row_count, dtype=jnp.int32)
    pooled = []
    for group_index in range(groups_here):
        running_sum = extended[:, group_index]
        window_span = 1
        while window_span < windows[group_index % 4]:
            running_sum = running_sum[window_span:] + running_sum[:-window_span]
            window_span = window_span * 2
        divisor = jnp.minimum(places + 1, window_span).astype(jnp.float32)[:, None]
        pooled.append(running_sum[running_sum.shape[0] - row_count :] / divisor)
    pooled = jnp.stack(pooled, axis=1)
    contrast = (pooled - extended[halo_reach:]).astype(jnp.bfloat16)
    first_group = lax.axis_index("tp") * groups_here
    maps_here = lax.dynamic_slice_in_dim(group_maps, first_group, groups_here, 0)
    mapped = jnp.einsum("sgc,gcd->sgd", contrast, maps_here, preferred_element_type=jnp.float32)
    scale_here = lax.dynamic_slice_in_dim(pool_scale, first_group * group_width, channels, 0)
    mixed_rows = (mapped.reshape(row_count, channels) * scale_here).astype(jnp.bfloat16)
    model_width = out_proj.shape[1]
    swapped = lax.all_to_all(mixed_rows, "tp", split_axis=0, concat_axis=1, tiled=True)
    projected = jnp.dot(swapped, out_proj, preferred_element_type=jnp.float32)
    settled = (residual.astype(jnp.float32) + projected).astype(jnp.bfloat16)
    settled_wide = settled.astype(jnp.float32)
    inverse_rms = lax.rsqrt(jnp.mean(settled_wide * settled_wide, axis=-1, keepdims=True) + epsilon)
    normed = (settled_wide * inverse_rms * norm_gain).astype(jnp.bfloat16)
    tokens_here, top_count = expert_ids.shape
    size_sp = lax.axis_size("sp")
    size_tp = lax.axis_size("tp")
    experts = size_sp * size_tp
    capacity = 3 * tokens_here * top_count // (2 * experts)
    cap = -(-capacity // 8) * 8
    layers = layer_count(size_sp)
    peers = experts // layers
    assigned = tokens_here * top_count
    flat_ids = expert_ids.reshape(assigned)
    onehot = (flat_ids[:, None] == jnp.arange(experts, dtype=jnp.int32)[None, :]).astype(
        jnp.bfloat16
    )
    earlier = (jnp.arange(assigned)[None, :] < jnp.arange(assigned)[:, None]).astype(jnp.bfloat16)
    before_counts = jnp.dot(earlier, onehot, preferred_element_type=jnp.float32)
    position = jnp.sum(before_counts * onehot, axis=1)
    slot = (flat_ids.astype(jnp.float32) * cap + position).reshape(tokens_here, top_count)
    weights = route_score / jnp.sum(route_score, axis=-1, keepdims=True) * routed_scale
    meta = jnp.concatenate([slot, weights], axis=1).T
    hidden_width = shared_gate.shape[1]
    expert_width = expert_gate.shape[2]
    any_spec = pl.BlockSpec(memory_space=pl.ANY)
    vmem_spec = pl.BlockSpec(memory_space=pltpu.VMEM)
    bf16, f32 = jnp.bfloat16, jnp.float32
    dma = pltpu.SemaphoreType.DMA
    routed = (layers, peers, cap, model_width)
    chunks = (layers, tokens_here, model_width)
    return pl.pallas_call(
        functools.partial(moe_kernel, layers, peers, size_tp, cap, top_count),
        out_shape=jax.ShapeDtypeStruct((tokens_here, model_width), bf16),
        in_specs=[vmem_spec] * 3 + [any_spec] * 6,
        out_specs=vmem_spec,
        scratch_shapes=[
            pltpu.VMEM(chunks, bf16),
            pltpu.VMEM((layers, 2 * top_count, tokens_here), f32),
            pltpu.VMEM(routed, bf16),
            pltpu.VMEM(routed, bf16),
            pltpu.VMEM(routed, bf16),
            pltpu.VMEM(routed, bf16),
            pltpu.VMEM(chunks, bf16),
            pltpu.VMEM(chunks, bf16),
            pltpu.VMEM((tokens_here, model_width), f32),
            pltpu.VMEM((model_width, hidden_width), bf16),
            pltpu.VMEM((model_width, hidden_width), bf16),
            pltpu.VMEM((hidden_width, model_width), bf16),
            pltpu.VMEM((model_width, expert_width), bf16),
            pltpu.VMEM((model_width, expert_width), bf16),
            pltpu.VMEM((expert_width, model_width), bf16),
            dma((6,)),
            dma((2,)),
            dma((2, layers)),
            dma((layers,)),
            dma((layers,)),
            dma((layers,)),
            dma((layers, peers)),
            dma((layers, peers)),
            dma((layers, peers)),
            dma((layers, peers)),
            dma((layers,)),
            dma((layers,)),
        ],
        compiler_params=pltpu.CompilerParams(
            collective_id=0, has_side_effects=True, vmem_limit_bytes=58 * 1024 * 1024
        ),
    )(
        normed,
        settled,
        meta,
        shared_gate,
        shared_up,
        shared_down,
        expert_gate,
        expert_up,
        expert_down,
    )


def solution(mesh):
    in_specs = (
        P(("sp", "tp"), None),
        P("sp", "tp"),
        P(),
        P(),
        P(),
        P(),
        P(),
        P(),
        P(),
        P(("sp", "tp"), None, None),
        P(("sp", "tp"), None, None),
        P(("sp", "tp"), None, None),
        P(("sp", "tp"), None),
        P(("sp", "tp"), None),
    )
    out_specs = P(("sp", "tp"), None)
    return jax.shard_map(
        on_device, mesh=mesh, in_specs=in_specs, out_specs=out_specs, check_vma=False
    )
```
